32 devices in a mesh: dp: 4 (over y, x), kv: 4 (over z), tp: 2 (over core).
Axes of the slice: x: 2, y: 2, z: 4, core: 2. Of those that a mesh axis runs over, the one named last changes fastest.
Arguments:
- tokens: bfloat16 [16, 4096], P('dp', 'kv'), may hold values from -24 to 24
- positions: int32 [16], P(('dp', 'kv')), may hold values from 0 to 4095
- state: float32 [16, 16, 128, 128], P(('dp', 'kv'), 'tp'), may hold values from -0.6 to 0.6
- w_query: bfloat16 [4096, 2048], P('kv', 'tp'), may hold values from -0.09375 to 0.09375
- w_key: bfloat16 [4096, 2048], P('kv', 'tp'), may hold values from -0.09375 to 0.09375
- w_value: bfloat16 [4096, 2048], P('kv', 'tp'), may hold values from -0.09375 to 0.09375
- w_gate: bfloat16 [4096, 2048], P('kv', 'tp'), may hold values from -0.09375 to 0.09375
- w_out: bfloat16 [2048, 4096], P(None, ('kv', 'tp')), may hold values from -0.25 to 0.25
- gain_mix: float32 [4096], replicated, may hold values from 0.1 to 1.9
- w_ffn_gate: bfloat16 [4096, 11008], P(None, ('kv', 'tp')), may hold values from -0.09375 to 0.09375
- w_ffn_up: bfloat16 [4096, 11008], P(None, ('kv', 'tp')), may hold values from -0.09375 to 0.09375
- w_ffn_down: bfloat16 [11008, 4096], P(('kv', 'tp')), may hold values from -0.109375 to 0.109375
- gain_out: float32 [4096], replicated, may hold values from 0.1 to 1.9
Outputs:
- layer_out: bfloat16 [16, 4096], P('dp', ('kv', 'tp'))
- new_state: float32 [16, 16, 128, 128], P(('dp', 'kv'), 'tp')
The draws below stay inside these ranges and needn't reach their ends.
All inputs are finite; a program needn't handle non-finite values.
Results may differ from the reference program's by a relative error of at most 0.018.
Values may be sent and summed in bfloat16 or wider, within the bound.
A program may use at most 128 MiB of HBM per device.

```python
import jax
import jax.numpy as jnp
from jax import lax

D = 4096
HEADS = 16
HEAD_DIM = 128
FF = 11008
BATCH = 16


def draw_tokens(key, part):
    normal_key = jax.random.fold_in(jax.random.fold_in(key, 11), 0)
    columns = jnp.arange(D, dtype=jnp.float32) / D
    column_scale = 0.5 * 4.0 ** columns
    base = jnp.clip(jax.random.normal(normal_key, (BATCH, D), jnp.float32), -6.0, 6.0)
    values = base * column_scale[None, :]
    return jnp.clip(values, -24.0, 24.0).astype(jnp.bfloat16)


def with_ends(entries, rng, least, top_value):
    shape = entries.shape
    place = [jax.random.randint(jax.random.fold_in(rng, axis), (), 0, shape[axis]) for axis in range(len(shape))]
    entries = entries.at[tuple(place)].set(least)
    longest = shape.index(max(shape))
    place[longest] = (place[longest] + 1) % shape[longest]
    return entries.at[tuple(place)].set(top_value)


def block_levels(own_key, dims, cuts, low, largest):
    def one(position, shards_of):
        steps = jax.random.uniform(jax.random.fold_in(jax.random.fold_in(own_key, 6), position), (shards_of,), jnp.float32, low / len(cuts), largest / len(cuts))
        return jnp.repeat(jnp.exp(steps), dims[position] // shards_of).reshape((-1,) + (1,) * (len(dims) - position - 1))

    level = one(*cuts[0])
    for cut in cuts[1:]:
        level = level * one(*cut)
    return level


def normal_values(rng, shape, scale, bound, cuts=(), held_as=jnp.bfloat16):
    values = jax.random.normal(rng, shape, jnp.float32) * scale
    if len(cuts) > 0:
        values = block_levels(rng, shape, cuts, -0.22, 0.18) * values
    return jnp.clip(values, min=-bound, max=bound).astype(held_as)


def setup_inputs(seed: int = 0) -> dict:
    seeds = jax.random.split(jax.random.key(seed), 14)
    return {
        "tokens": draw_tokens(jax.random.fold_in(seeds[13], 71), 0),
        "positions": with_ends(jax.random.randint(seeds[1], (BATCH,), 0, 4096), jax.random.fold_in(seeds[1], 1), 0, 4095).astype(jnp.int32),
        "state": normal_values(seeds[2], (BATCH, HEADS, HEAD_DIM, HEAD_DIM), 0.1, 0.6, ((0, 16), (1, 2)), jnp.float32),
        "w_query": normal_values(seeds[3], (D, HEADS * HEAD_DIM), D ** -0.5, 0.09375, ((0, 4), (1, 2))),
        "w_key": normal_values(seeds[4], (D, HEADS * HEAD_DIM), D ** -0.5, 0.09375, ((0, 4), (1, 2))),
        "w_value": normal_values(seeds[5], (D, HEADS * HEAD_DIM), D ** -0.5, 0.09375, ((0, 4), (1, 2))),
        "w_gate": normal_values(seeds[6], (D, HEADS * HEAD_DIM), D ** -0.5, 0.09375, ((0, 4), (1, 2))),
        "w_out": normal_values(seeds[7], (HEADS * HEAD_DIM, D), (HEADS * HEAD_DIM // 4) ** -0.5, 0.25, ((1, 8),)),
        "gain_mix": jnp.clip(1.0 + 0.18 * jax.random.normal(seeds[8], (D,), jnp.float32), 0.1, 1.9),
        "w_ffn_gate": normal_values(seeds[9], (D, FF), D ** -0.5, 0.09375, ((1, 8),)),
        "w_ffn_up": normal_values(seeds[10], (D, FF), D ** -0.5, 0.09375, ((1, 8),)),
        "w_ffn_down": normal_values(seeds[11], (FF, D), (FF // 4) ** -0.5, 0.109375, ((0, 8),)),
        "gain_out": jnp.clip(1.0 + 0.18 * jax.random.normal(seeds[12], (D,), jnp.float32), 0.1, 1.9),
    }


def rotate(vectors, positions):
    half = vectors.shape[-1] // 2
    inverse = 10000.0 ** (-jnp.arange(half, dtype=jnp.float32) / half)
    angle = positions.astype(jnp.float32)[:, None, None] * inverse[None, None, :]
    cosine = jnp.cos(angle)
    sine = jnp.sin(angle)
    first = vectors[..., :half]
    second = vectors[..., half:]
    return jnp.concatenate([first * cosine - second * sine, first * sine + second * cosine], -1)

def layer_norm(values, gain):
    count = values.shape[-1]
    mean = lax.optimization_barrier(jnp.sum(values, -1, keepdims=True)) / count
    var = lax.optimization_barrier(jnp.sum(values * values, -1, keepdims=True)) / count - mean * mean
    return (values - mean) * lax.rsqrt(var + 1e-05) * gain

def reference(tokens, positions, state, w_query, w_key, w_value, w_gate, w_out, gain_mix, w_ffn_gate, w_ffn_up, w_ffn_down, gain_out):
    rows = tokens.shape[0]
    heads = state.shape[1]
    width_head = state.shape[2]
    query = jnp.dot(tokens, w_query, preferred_element_type=jnp.float32).reshape(rows, heads, width_head)
    key = jnp.dot(tokens, w_key, preferred_element_type=jnp.float32).reshape(rows, heads, width_head)
    value = jnp.dot(tokens, w_value, preferred_element_type=jnp.float32).reshape(rows, heads, width_head)
    gate_pre = jnp.dot(tokens, w_gate, preferred_element_type=jnp.float32)
    query = rotate(query, positions)
    key = rotate(key, positions) * width_head ** (-0.5)
    head_ids = jnp.arange(heads, dtype=jnp.float32)
    decay = 1.0 - 2.0 ** (-5.0 - 6.0 * head_ids / (heads - 1))
    new_state = decay[None, :, None, None] * state + key[:, :, :, None] * value[:, :, None, :]
    retained = jnp.einsum('bhd,bhdv->bhv', query, new_state, precision=lax.Precision.HIGHEST)
    mean = lax.optimization_barrier(jnp.mean(retained, -1, keepdims=True))
    var = lax.optimization_barrier(jnp.mean(jnp.square(retained - mean), -1, keepdims=True))
    normed = (retained - mean) * lax.rsqrt(var + 1e-05)
    attended = (normed.reshape(rows, heads * width_head) * jax.nn.silu(gate_pre)).astype(jnp.bfloat16)
    mixed = jnp.dot(attended, w_out, preferred_element_type=jnp.float32)
    mixed_pre = (tokens.astype(jnp.float32) + mixed).astype(jnp.bfloat16)
    hidden = layer_norm(mixed_pre.astype(jnp.float32), gain_mix).astype(jnp.bfloat16)
    gate = jnp.dot(hidden, w_ffn_gate, preferred_element_type=jnp.float32)
    upward = jnp.dot(hidden, w_ffn_up, preferred_element_type=jnp.float32)
    inner = (jax.nn.silu(gate) * upward).astype(jnp.bfloat16)
    ffn = jnp.dot(inner, w_ffn_down, preferred_element_type=jnp.float32)
    layer_out = layer_norm(hidden.astype(jnp.float32) + ffn, gain_out).astype(jnp.bfloat16)
    return (layer_out, new_state)
```

```python
import functools

import jax
import jax.numpy as jnp
import numpy as np
from jax import lax
from jax.experimental import pallas as pl
from jax.experimental.pallas import tpu as pltpu
from jax.sharding import PartitionSpec as P

MESH = pl.DeviceIdType.MESH
F32 = jnp.float32
BF16 = jnp.bfloat16


def dot_rows(values, weight):
    return lax.dot_general(values, weight, (((1,), (1,)), ((), ())), preferred_element_type=F32)


def step_kernel(
    kv_count,
    tp_count,
    tok_h,
    pos_s,
    state_h,
    wq_h,
    wk_h,
    wv_h,
    wg_h,
    wout_h,
    gmix_h,
    wfg_h,
    wfu_h,
    wfd_h,
    gout_h,
    inv_h,
    out_v,
    nst_h,
    tok,
    state,
    nst,
    wq,
    wk,
    wv,
    wg,
    wout,
    gmix,
    wfg,
    wfu,
    wfd,
    gout,
    inv,
    qsend,
    qrecv,
    att,
    mix,
    hid_own,
    hid,
    inner,
    fsend,
    frecv,
    sums,
    local_sem,
    q_send_sem,
    q_recv_sem,
    send_sem,
    recv_sem,
):
    group = kv_count * tp_count
    dp = lax.axis_index("dp")
    kv = lax.axis_index("kv")
    tp = lax.axis_index("tp")
    me = kv * tp_count + tp
    rows = tok.shape[0]
    heads = state.shape[0]
    width_head = state.shape[1]
    width = hid.shape[1]
    cols = mix.shape[2]
    ff = wfg.shape[0]

    far = sorted(range(1, kv_count), key=lambda d: -min(d, kv_count - d))
    steps = [(d, e) for d in far for e in range(tp_count)]
    steps += [(0, e) for e in range(1, tp_count)]

    def partner(d, e):
        return lax.rem(kv + d, kv_count), lax.rem(tp + e, tp_count)

    barrier = pltpu.get_barrier_semaphore()
    for d, e in steps:
        other_kv, other_tp = partner(d, e)
        pl.semaphore_signal(
            barrier, inc=1, device_id=(dp, other_kv, other_tp), device_id_type=MESH
        )

    loads = []

    def load(src, dst):
        copy = pltpu.make_async_copy(src, dst, local_sem.at[len(loads)])
        copy.start()
        loads.append(copy)
        return copy

    tok_load = load(tok_h, tok)
    inv_load = load(inv_h, inv)
    proj_loads = [
        load(src, dst) for src, dst in ((wq_h, wq), (wk_h, wk), (wv_h, wv), (wg_h, wg))
    ]
    state_load = load(state_h, state)
    gmix_load = load(gmix_h, gmix)
    gout_load = load(gout_h, gout)

    inv_load.wait()
    lane = lax.broadcasted_iota(jnp.int32, (1, width_head), 1)
    angle = pos_s[0].astype(F32) * inv[...]
    cosine = jnp.cos(angle)
    sine = jnp.sin(angle)
    sine = jnp.where(lane < width_head // 2, -sine, sine)

    tok_load.wait()
    pl.semaphore_wait(barrier, group - 1)
    later = []
    q_copies = []
    for p, weight in enumerate((wq, wk, wv, wg)):
        proj_loads[p].wait()
        if p == 0:
            later.append(load(wout_h, wout))
        elif p == 1:
            later.append(load(wfg_h, wfg))
        elif p == 2:
            later.append(load(wfu_h, wfu))
        else:
            later.append(load(wfd_h, wfd))
        part = jnp.dot(tok[...], weight[...], preferred_element_type=F32)
        for i in range(kv_count):
            for h in range(heads):
                qsend[i, p, h : h + 1, :] = part[
                    i : i + 1, h * width_head : (h + 1) * width_head
                ]
        for d in far:
            other_kv, _ = partner(d, 0)
            copy = pltpu.make_async_remote_copy(
                src_ref=qsend.at[other_kv, p],
                dst_ref=qrecv.at[kv, p],
                send_sem=q_send_sem.at[p, d],
                recv_sem=q_recv_sem.at[p, d],
                device_id=(dp, other_kv, tp),
                device_id_type=MESH,
            )
            copy.start()
            q_copies.append((p, d, copy))
    wout_load, wfg_load, wfu_load, wfd_load = later

    head_id = (tp * heads + lax.broadcasted_iota(jnp.int32, (heads, width_head), 0)).astype(F32)
    total_heads = heads * tp_count
    decay = 1.0 - jnp.exp2(-5.0 - 6.0 * head_id / (total_heads - 1))

    def rotate_row(x):
        return x * cosine + pltpu.roll(x, width_head // 2, 1) * sine

    projected = []
    for p in range(4):
        total = qsend[kv, p]
        for q, d, copy in q_copies:
            if q == p:
                copy.wait_recv()
                total = total + qrecv[lax.rem(kv + kv_count - d, kv_count), p]
        projected.append(total)
    query, key, value, gate_pre = projected
    query = rotate_row(query)
    key = rotate_row(key) * width_head ** (-0.5)
    query_t = jnp.transpose(query)
    key_t = jnp.transpose(key)
    state_load.wait()
    retained = []
    for h in range(heads):
        new = decay[h : h + 1, :] * state[h] + key_t[:, h : h + 1] * value[h : h + 1, :]
        nst[h] = new
        retained.append(jnp.sum(query_t[:, h : h + 1] * new, axis=0, keepdims=True))
    retained = jnp.concatenate(retained, axis=0)
    mean = jnp.mean(retained, -1, keepdims=True)
    var = jnp.mean(jnp.square(retained - mean), -1, keepdims=True)
    normed = (retained - mean) * lax.rsqrt(var + 1e-05)
    silu_gate = gate_pre / (1.0 + jnp.exp(-gate_pre))
    attended = (normed * silu_gate).astype(BF16).astype(F32)
    own_rows = pl.ds(pl.multiple_of(me * heads, heads), heads)
    att[own_rows, :] = attended

    def send_all(phase, src, dst):
        copies = []
        for d, e in steps:
            other_kv, other_tp = partner(d, e)
            copy = pltpu.make_async_remote_copy(
                src_ref=src,
                dst_ref=dst,
                send_sem=send_sem.at[phase, d * tp_count + e],
                recv_sem=recv_sem.at[phase, d * tp_count + e],
                device_id=(dp, other_kv, other_tp),
                device_id_type=MESH,
            )
            copy.start()
            copies.append(copy)
        return copies

    att_copies = send_all(0, att.at[own_rows, :], att.at[own_rows, :])
    nst_store = pltpu.make_async_copy(nst, nst_h, local_sem.at[len(loads)])
    nst_store.start()

    wout_load.wait()
    for copy in att_copies:
        copy.wait_recv()
    lhs = jnp.concatenate(
        [
            att[pl.ds(t * heads + h, rows, stride=tp_count * heads), :]
            for t in range(tp_count)
            for h in range(heads)
        ],
        axis=1,
    ).astype(BF16)
    mixed = jnp.dot(lhs, wout[...], preferred_element_type=F32)
    tok_own = tok[:, pl.ds(pl.multiple_of(tp * cols, cols), cols)]
    mix[me] = (tok_own.astype(F32) + mixed).astype(BF16).astype(F32)
    mix_copies = send_all(1, mix.at[me], mix.at[me])
    gmix_load.wait()
    gout_load.wait()
    for copy in mix_copies:
        copy.wait_recv()
    whole = [mix[p] for p in range(group)]
    total = functools.reduce(lambda a, b: a + b, whole)
    squares = functools.reduce(lambda a, b: a + b, [x * x for x in whole])
    mean = jnp.sum(total, 1, keepdims=True) / width
    var = jnp.sum(squares, 1, keepdims=True) / width - mean * mean
    scale = lax.rsqrt(var + 1e-05)
    for p in range(group):
        block = slice(p * cols, (p + 1) * cols)
        hidden = ((whole[p] - mean) * scale * gmix[:, block]).astype(BF16)
        hid[:, block] = hidden
        hid_own[p] = hidden.astype(F32)

    wfg_load.wait()
    wfu_load.wait()
    tile = 256
    whole_tiles = ff // tile

    def inner_block(at):
        gate = dot_rows(hid[...], wfg[at, :])
        upward = dot_rows(hid[...], wfu[at, :])
        inner[:, at] = (gate / (1.0 + jnp.exp(-gate)) * upward).astype(BF16)

    @pl.loop(0, whole_tiles)
    def _(j):
        inner_block(pl.ds(pl.multiple_of(j * tile, tile), tile))

    if ff % tile:
        inner_block(pl.ds(whole_tiles * tile, ff % tile))

    wfd_load.wait()
    main = ff // 128 * 128

    def down_block(owner):
        at = pl.ds(pl.multiple_of(owner * cols, cols), cols)
        result = jnp.dot(inner[:, :main], wfd[:main, at], preferred_element_type=F32)
        if main < ff:
            result += jnp.dot(inner[:, main:], wfd[main:, at], preferred_element_type=F32)
        return result

    f_copies = []
    for d, e in steps:
        other_kv, other_tp = partner(d, e)
        owner = other_kv * tp_count + other_tp
        fsend[owner] = down_block(owner)
        copy = pltpu.make_async_remote_copy(
            src_ref=fsend.at[owner],
            dst_ref=frecv.at[me],
            send_sem=send_sem.at[2, d * tp_count + e],
            recv_sem=recv_sem.at[2, d * tp_count + e],
            device_id=(dp, other_kv, other_tp),
            device_id_type=MESH,
        )
        copy.start()
        f_copies.append((d, e, copy))
    summed = hid_own[me] + down_block(me)
    for d, e, copy in f_copies:
        copy.wait_recv()
        source = lax.rem(kv + kv_count - d, kv_count) * tp_count + lax.rem(
            tp + tp_count - e, tp_count
        )
        summed = summed + frecv[source]
    own_sum = jnp.sum(summed, 1, keepdims=True)
    own_square = jnp.sum(summed * summed, 1, keepdims=True)
    sums[me, 0] = jnp.broadcast_to(own_sum, (rows, 128))
    sums[me, 1] = jnp.broadcast_to(own_square, (rows, 128))
    sum_copies = send_all(3, sums.at[me], sums.at[me])
    for copy in sum_copies:
        copy.wait_recv()
    all_sum = functools.reduce(lambda a, b: a + b, [sums[p, 0] for p in range(group)])
    all_square = functools.reduce(lambda a, b: a + b, [sums[p, 1] for p in range(group)])
    mean = all_sum[:, :1] / width
    var = all_square[:, :1] / width - mean * mean
    gain = gout[:, pl.ds(pl.multiple_of(me * cols, cols), cols)]
    out_v[...] = ((summed - mean) * lax.rsqrt(var + 1e-05) * gain).astype(BF16)

    for _, _, copy in q_copies:
        copy.wait_send()
    for copies in (att_copies, mix_copies, sum_copies):
        for copy in copies:
            copy.wait_send()
    for _, _, copy in f_copies:
        copy.wait_send()
    nst_store.wait()


def fused_step(
    tokens,
    positions,
    state,
    w_query,
    w_key,
    w_value,
    w_gate,
    w_out,
    gain_mix,
    w_ffn_gate,
    w_ffn_up,
    w_ffn_down,
    gain_out,
):
    kv_count = lax.axis_size("kv")
    tp_count = lax.axis_size("tp")
    group = kv_count * tp_count
    rows = tokens.shape[0]
    _, heads, width_head, _ = state.shape
    width = w_ffn_gate.shape[0]
    cols = w_out.shape[1]
    half = width_head // 2
    inverse = 10000.0 ** (-np.arange(half, dtype=np.float32) / half)
    inverse = np.tile(inverse.astype(np.float32), 2)[None, :]
    arrays = (
        tokens,
        state[0],
        w_query,
        w_key,
        w_value,
        w_gate,
        w_out,
        gain_mix[None, :],
        w_ffn_gate.T,
        w_ffn_up.T,
        w_ffn_down,
        gain_out[None, :],
        jnp.asarray(inverse),
    )
    held = [pltpu.VMEM(a.shape, a.dtype) for a in arrays]
    held.insert(2, pltpu.VMEM(arrays[1].shape, F32))
    any_spec = pl.BlockSpec(memory_space=pl.ANY)
    out, new_state = pl.pallas_call(
        functools.partial(step_kernel, kv_count, tp_count),
        out_shape=(
            jax.ShapeDtypeStruct((rows, cols), BF16),
            jax.ShapeDtypeStruct(arrays[1].shape, F32),
        ),
        in_specs=[any_spec, pl.BlockSpec(memory_space=pltpu.SMEM)] + [any_spec] * 12,
        out_specs=(pl.BlockSpec(memory_space=pltpu.VMEM), any_spec),
        scratch_shapes=held
        + [
            pltpu.VMEM((kv_count, 4, heads, width_head), F32),
            pltpu.VMEM((kv_count, 4, heads, width_head), F32),
            pltpu.VMEM((group * heads, width_head), F32),
            pltpu.VMEM((group, rows, cols), F32),
            pltpu.VMEM((group, rows, cols), F32),
            pltpu.VMEM((rows, width), BF16),
            pltpu.VMEM((rows, w_ffn_gate.shape[1]), BF16),
            pltpu.VMEM((group, rows, cols), F32),
            pltpu.VMEM((group, rows, cols), F32),
            pltpu.VMEM((group, 2, rows, 128), F32),
            pltpu.SemaphoreType.DMA((len(arrays) + 1,)),
            pltpu.SemaphoreType.DMA((4, kv_count)),
            pltpu.SemaphoreType.DMA((4, kv_count)),
            pltpu.SemaphoreType.DMA((4, group)),
            pltpu.SemaphoreType.DMA((4, group)),
        ],
        compiler_params=pltpu.CompilerParams(
            collective_id=0, has_side_effects=True, vmem_limit_bytes=60 * 1024 * 1024
        ),
    )(arrays[0], positions, *arrays[1:])
    return out, new_state[None]


def fits_kernel(tokens, state, w_out, kv_count, tp_count):
    seqs, _, width_head, _ = state.shape
    return (
        seqs == 1
        and width_head == 128
        and w_out.shape[1] % 128 == 0
        and tokens.shape[0] == kv_count
        and kv_count * tp_count <= 16
    )


def rotate(vectors, positions):
    half = vectors.shape[-1] // 2
    inverse = 10000.0 ** (-jnp.arange(half, dtype=jnp.float32) / half)
    angle = positions.astype(jnp.float32)[:, None, None] * inverse[None, None, :]
    cosine = jnp.cos(angle)
    sine = jnp.sin(angle)
    first = vectors[..., :half]
    second = vectors[..., half:]
    return jnp.concatenate([first * cosine - second * sine, first * sine + second * cosine], -1)


def finish_norm(values, sums, squares, count, gain):
    mean = sums / count
    var = squares / count - mean * mean
    return (values - mean[:, None]) * lax.rsqrt(var + 1e-05)[:, None] * gain[None, :]


def on_device(
    tokens,
    positions,
    state,
    w_query,
    w_key,
    w_value,
    w_gate,
    w_out,
    gain_mix,
    w_ffn_gate,
    w_ffn_up,
    w_ffn_down,
    gain_out,
):
    if fits_kernel(tokens, state, w_out, lax.axis_size("kv"), lax.axis_size("tp")):
        return fused_step(
            tokens,
            positions,
            state,
            w_query,
            w_key,
            w_value,
            w_gate,
            w_out,
            gain_mix,
            w_ffn_gate,
            w_ffn_up,
            w_ffn_down,
            gain_out,
        )
    seqs = state.shape[0]
    heads = state.shape[1]
    width_head = state.shape[2]
    proj_cols = w_query.shape[1]
    width = w_ffn_gate.shape[0]
    cols = w_out.shape[1]
    group_rows = tokens.shape[0]
    kv_count = lax.axis_size("kv")
    tp_count = lax.axis_size("tp")
    tp_index = lax.axis_index("tp")
    col_start = (lax.axis_index("kv") * tp_count + tp_index) * cols
    projected = lax.psum_scatter(
        jnp.concatenate(
            [
                jnp.dot(tokens, w_query, preferred_element_type=jnp.float32),
                jnp.dot(tokens, w_key, preferred_element_type=jnp.float32),
                jnp.dot(tokens, w_value, preferred_element_type=jnp.float32),
                jnp.dot(tokens, w_gate, preferred_element_type=jnp.float32),
            ],
            axis=1,
        ),
        "kv",
        scatter_dimension=0,
        tiled=True,
    )
    query = projected[:, :proj_cols].reshape(seqs, heads, width_head)
    key = projected[:, proj_cols : 2 * proj_cols].reshape(seqs, heads, width_head)
    value = projected[:, 2 * proj_cols : 3 * proj_cols].reshape(seqs, heads, width_head)
    gate_pre = projected[:, 3 * proj_cols :]
    query = rotate(query, positions)
    key = rotate(key, positions) * width_head ** (-0.5)
    total_heads = heads * tp_count
    head_ids = (tp_index * heads + jnp.arange(heads, dtype=jnp.int32)).astype(jnp.float32)
    decay = 1.0 - 2.0 ** (-5.0 - 6.0 * head_ids / (total_heads - 1))
    new_state = decay[None, :, None, None] * state + key[:, :, :, None] * value[:, :, None, :]
    retained = jnp.einsum("bhd,bhdv->bhv", query, new_state, precision=lax.Precision.HIGHEST)
    mean = jnp.mean(retained, -1, keepdims=True)
    var = jnp.mean(jnp.square(retained - mean), -1, keepdims=True)
    normed = (retained - mean) * lax.rsqrt(var + 1e-05)
    attended = (normed.reshape(seqs, proj_cols) * jax.nn.silu(gate_pre)).astype(jnp.bfloat16)
    gathered = lax.all_gather(attended[None], ("kv", "tp"), axis=0, tiled=True)
    gathered = gathered.reshape(kv_count, tp_count, seqs, proj_cols)
    out_blocks = w_out.reshape(tp_count, proj_cols, cols)
    mixed = jnp.einsum(
        "itsc,tcd->isd", gathered, out_blocks, preferred_element_type=jnp.float32
    ).reshape(group_rows, cols)
    tokens_own = lax.dynamic_slice_in_dim(tokens, tp_index * cols, cols, 1)
    mixed_pre = (tokens_own.astype(jnp.float32) + mixed).astype(jnp.bfloat16)
    gain_out_own = lax.dynamic_slice_in_dim(gain_out, col_start, cols, 0)
    whole_rows = lax.all_gather(mixed_pre, ("kv", "tp"), axis=1, tiled=True).astype(jnp.float32)
    hidden = finish_norm(
        whole_rows, jnp.sum(whole_rows, 1), jnp.sum(whole_rows * whole_rows, 1), width, gain_mix
    ).astype(jnp.bfloat16)
    hidden_own = lax.dynamic_slice_in_dim(hidden, col_start, cols, 1)
    gate = jnp.dot(hidden, w_ffn_gate, preferred_element_type=jnp.float32)
    upward = jnp.dot(hidden, w_ffn_up, preferred_element_type=jnp.float32)
    inner = (jax.nn.silu(gate) * upward).astype(jnp.bfloat16)
    ffn_cols = lax.psum_scatter(
        lax.dot_general(
            w_ffn_down, inner, (((0,), (1,)), ((), ())), preferred_element_type=jnp.float32
        ),
        ("kv", "tp"),
        scatter_dimension=0,
        tiled=True,
    )
    summed = hidden_own.astype(jnp.float32) + ffn_cols.T
    out_sums, out_squares = lax.psum(
        (jnp.sum(summed, 1), jnp.sum(summed * summed, 1)), ("kv", "tp")
    )
    layer_out = finish_norm(summed, out_sums, out_squares, width, gain_out_own).astype(jnp.bfloat16)
    return (layer_out, new_state)


def solution(mesh):
    return jax.shard_map(
        on_device,
        mesh=mesh,
        in_specs=(
            P("dp", "kv"),
            P(("dp", "kv")),
            P(("dp", "kv"), "tp", None, None),
            P("kv", "tp"),
            P("kv", "tp"),
            P("kv", "tp"),
            P("kv", "tp"),
            P(None, ("kv", "tp")),
            P(),
            P(None, ("kv", "tp")),
            P(None, ("kv", "tp")),
            P(("kv", "tp"), None),
            P(),
        ),
        out_specs=(P("dp", ("kv", "tp")), P(("dp", "kv"), "tp", None, None)),
        check_vma=False,
    )
```

```python
import functools

import jax
import jax.numpy as jnp
import numpy as np
from jax import lax
from jax.experimental import pallas as pl
from jax.experimental.pallas import tpu as pltpu
from jax.sharding import PartitionSpec as P

MESH = pl.DeviceIdType.MESH
F32 = jnp.float32
BF16 = jnp.bfloat16


def dot_rows(values, weight):
    return lax.dot_general(values, weight, (((1,), (1,)), ((), ())), preferred_element_type=F32)


def step_kernel(
    kv_count,
    tp_count,
    tok_h,
    pos_h,
    state_h,
    wq_h,
    wk_h,
    wv_h,
    wg_h,
    wout_h,
    gmix_h,
    wfg_h,
    wfu_h,
    wfd_h,
    gout_h,
    inv_h,
    out_v,
    nst,
    tok,
    pos,
    state,
    wq,
    wk,
    wv,
    wg,
    wout,
    gmix,
    wfg,
    wfu,
    wfd,
    gout,
    inv,
    qsend,
    qrecv,
    att,
    mix,
    hid_own,
    hid,
    inner,
    fsend,
    frecv,
    sums,
    local_sem,
    q_send_sem,
    q_recv_sem,
    send_sem,
    recv_sem,
):
    group = kv_count * tp_count
    dp = lax.axis_index("dp")
    kv = lax.axis_index("kv")
    tp = lax.axis_index("tp")
    me = kv * tp_count + tp
    rows = tok.shape[0]
    heads = state.shape[0]
    width_head = state.shape[1]
    width = hid.shape[1]
    cols = mix.shape[2]
    ff = wfg.shape[0]

    far = sorted(range(1, kv_count), key=lambda d: -min(d, kv_count - d))
    steps = [(d, e) for d in far for e in range(tp_count)]
    steps += [(0, e) for e in range(1, tp_count)]

    def partner(d, e):
        return lax.rem(kv + d, kv_count), lax.rem(tp + e, tp_count)

    barrier = pltpu.get_barrier_semaphore()
    for d, e in steps:
        other_kv, other_tp = partner(d, e)
        pl.semaphore_signal(
            barrier, inc=1, device_id=(dp, other_kv, other_tp), device_id_type=MESH
        )

    loads = []

    def load(src, dst):
        copy = pltpu.make_async_copy(src, dst, local_sem.at[len(loads)])
        copy.start()
        loads.append(copy)
        return copy

    tok_load = load(tok_h, tok)
    pos_load = load(pos_h, pos)
    inv_load = load(inv_h, inv)
    proj_loads = [
        load(src, dst) for src, dst in ((wq_h, wq), (wk_h, wk), (wv_h, wv), (wg_h, wg))
    ]
    state_load = load(state_h, state)
    gmix_load = load(gmix_h, gmix)
    gout_load = load(gout_h, gout)

    pos_load.wait()
    inv_load.wait()
    lane = lax.broadcasted_iota(jnp.int32, (1, width_head), 1)
    angle = pos[...].astype(F32) * inv[...]
    cosine = jnp.cos(angle)
    sine = jnp.sin(angle)
    sine = jnp.where(lane < width_head // 2, -sine, sine)

    tok_load.wait()
    pl.semaphore_wait(barrier, group - 1)
    later = []
    q_copies = []
    for p, weight in enumerate((wq, wk, wv, wg)):
        proj_loads[p].wait()
        if p == 0:
            later.append(load(wout_h, wout))
        elif p == 1:
            later.append(load(wfg_h, wfg))
        elif p == 2:
            later.append(load(wfu_h, wfu))
        else:
            later.append(load(wfd_h, wfd))
        part = jnp.dot(tok[...], weight[...], preferred_element_type=F32)
        for i in range(kv_count):
            for h in range(heads):
                qsend[i, p, h : h + 1, :] = part[
                    i : i + 1, h * width_head : (h + 1) * width_head
                ]
        for d in far:
            other_kv, _ = partner(d, 0)
            copy = pltpu.make_async_remote_copy(
                src_ref=qsend.at[other_kv, p],
                dst_ref=qrecv.at[kv, p],
                send_sem=q_send_sem.at[p, d],
                recv_sem=q_recv_sem.at[p, d],
                device_id=(dp, other_kv, tp),
                device_id_type=MESH,
            )
            copy.start()
            q_copies.append((p, d, copy))
    wout_load, wfg_load, wfu_load, wfd_load = later

    head_id = (tp * heads + lax.broadcasted_iota(jnp.int32, (heads, width_head), 0)).astype(F32)
    total_heads = heads * tp_count
    decay = 1.0 - jnp.exp2(-5.0 - 6.0 * head_id / (total_heads - 1))

    def rotate_row(x):
        return x * cosine + pltpu.roll(x, width_head // 2, 1) * sine

    projected = []
    for p in range(4):
        total = qsend[kv, p]
        for q, d, copy in q_copies:
            if q == p:
                copy.wait_recv()
                total = total + qrecv[lax.rem(kv + kv_count - d, kv_count), p]
        projected.append(total)
    query, key, value, gate_pre = projected
    query = rotate_row(query)
    key = rotate_row(key) * width_head ** (-0.5)
    query_t = jnp.transpose(query)
    key_t = jnp.transpose(key)
    state_load.wait()
    retained = []
    for h in range(heads):
        new = decay[h : h + 1, :] * state[h] + key_t[:, h : h + 1] * value[h : h + 1, :]
        nst[h] = new
        retained.append(jnp.sum(query_t[:, h : h + 1] * new, axis=0, keepdims=True))
    retained = jnp.concatenate(retained, axis=0)
    mean = jnp.mean(retained, -1, keepdims=True)
    var = jnp.mean(jnp.square(retained - mean), -1, keepdims=True)
    normed = (retained - mean) * lax.rsqrt(var + 1e-05)
    silu_gate = gate_pre / (1.0 + jnp.exp(-gate_pre))
    attended = (normed * silu_gate).astype(BF16).astype(F32)
    own_rows = pl.ds(pl.multiple_of(me * heads, heads), heads)
    att[own_rows, :] = attended

    def send_all(phase, src, dst):
        copies = []
        for d, e in steps:
            other_kv, other_tp = partner(d, e)
            copy = pltpu.make_async_remote_copy(
                src_ref=src,
                dst_ref=dst,
                send_sem=send_sem.at[phase, d * tp_count + e],
                recv_sem=recv_sem.at[phase, d * tp_count + e],
                device_id=(dp, other_kv, other_tp),
                device_id_type=MESH,
            )
            copy.start()
            copies.append(copy)
        return copies

    att_copies = send_all(0, att.at[own_rows, :], att.at[own_rows, :])

    wout_load.wait()
    for copy in att_copies:
        copy.wait_recv()
    lhs = jnp.concatenate(
        [
            att[pl.ds(t * heads + h, rows, stride=tp_count * heads), :]
            for t in range(tp_count)
            for h in range(heads)
        ],
        axis=1,
    ).astype(BF16)
    mixed = jnp.dot(lhs, wout[...], preferred_element_type=F32)
    tok_own = tok[:, pl.ds(pl.multiple_of(tp * cols, cols), cols)]
    mix[me] = (tok_own.astype(F32) + mixed).astype(BF16)
    mix_copies = send_all(1, mix.at[me], mix.at[me])
    gmix_load.wait()
    gout_load.wait()
    for copy in mix_copies:
        copy.wait_recv()
    whole = [mix[p].astype(F32) for p in range(group)]
    total = functools.reduce(lambda a, b: a + b, whole)
    squares = functools.reduce(lambda a, b: a + b, [x * x for x in whole])
    mean = jnp.sum(total, 1, keepdims=True) / width
    var = jnp.sum(squares, 1, keepdims=True) / width - mean * mean
    scale = lax.rsqrt(var + 1e-05)
    for p in range(group):
        block = slice(p * cols, (p + 1) * cols)
        hidden = ((whole[p] - mean) * scale * gmix[:, block]).astype(BF16)
        hid[:, block] = hidden
        hid_own[p] = hidden.astype(F32)

    wfg_load.wait()
    wfu_load.wait()
    tile = 256
    whole_tiles = ff // tile

    def inner_block(at):
        gate = dot_rows(hid[...], wfg[at, :])
        upward = dot_rows(hid[...], wfu[at, :])
        inner[:, at] = (gate / (1.0 + jnp.exp(-gate)) * upward).astype(BF16)

    for j in range(whole_tiles):
        inner_block(pl.ds(j * tile, tile))

    if ff % tile:
        inner_block(pl.ds(whole_tiles * tile, ff % tile))

    wfd_load.wait()
    main = ff // 128 * 128

    def down_block(owner):
        at = pl.ds(pl.multiple_of(owner * cols, cols), cols)
        result = jnp.dot(inner[:, :main], wfd[:main, at], preferred_element_type=F32)
        if main < ff:
            result += jnp.dot(inner[:, main:], wfd[main:, at], preferred_element_type=F32)
        return result

    f_copies = []
    for d, e in steps:
        other_kv, other_tp = partner(d, e)
        owner = other_kv * tp_count + other_tp
        fsend[owner] = down_block(owner).astype(BF16)
        copy = pltpu.make_async_remote_copy(
            src_ref=fsend.at[owner],
            dst_ref=frecv.at[me],
            send_sem=send_sem.at[2, d * tp_count + e],
            recv_sem=recv_sem.at[2, d * tp_count + e],
            device_id=(dp, other_kv, other_tp),
            device_id_type=MESH,
        )
        copy.start()
        f_copies.append((d, e, copy))
    summed = hid_own[me] + down_block(me)
    for d, e, copy in f_copies:
        copy.wait_recv()
        source = lax.rem(kv + kv_count - d, kv_count) * tp_count + lax.rem(
            tp + tp_count - e, tp_count
        )
        summed = summed + frecv[source].astype(F32)
    own_sum = jnp.sum(summed, 1, keepdims=True)
    own_square = jnp.sum(summed * summed, 1, keepdims=True)
    low_half = lax.broadcasted_iota(jnp.int32, (rows, 128), 1) < 64
    sums[me] = jnp.where(low_half, own_sum, own_square)
    sum_copies = send_all(3, sums.at[me], sums.at[me])
    for copy in sum_copies:
        copy.wait_recv()
    all_sums = functools.reduce(lambda a, b: a + b, [sums[p] for p in range(group)])
    mean = all_sums[:, :1] / width
    var = all_sums[:, 64:65] / width - mean * mean
    gain = gout[:, pl.ds(pl.multiple_of(me * cols, cols), cols)]
    out_v[...] = ((summed - mean) * lax.rsqrt(var + 1e-05) * gain).astype(BF16)

    for _, _, copy in q_copies:
        copy.wait_send()
    for copies in (att_copies, mix_copies, sum_copies):
        for copy in copies:
            copy.wait_send()
    for _, _, copy in f_copies:
        copy.wait_send()


def store_kernel(out_v, nst_v, out_h, nst_h, sem):
    copies = [
        pltpu.make_async_copy(nst_v, nst_h, sem.at[0]),
        pltpu.make_async_copy(out_v, out_h, sem.at[1]),
    ]
    for copy in copies:
        copy.start()
    for copy in copies:
        copy.wait()


def fused_step(
    tokens,
    positions,
    state,
    w_query,
    w_key,
    w_value,
    w_gate,
    w_out,
    gain_mix,
    w_ffn_gate,
    w_ffn_up,
    w_ffn_down,
    gain_out,
):
    kv_count = lax.axis_size("kv")
    tp_count = lax.axis_size("tp")
    group = kv_count * tp_count
    rows = tokens.shape[0]
    _, heads, width_head, _ = state.shape
    width = w_ffn_gate.shape[0]
    cols = w_out.shape[1]
    half = width_head // 2
    inverse = 10000.0 ** (-np.arange(half, dtype=np.float32) / half)
    inverse = np.tile(inverse.astype(np.float32), 2)[None, :]
    arrays = (
        tokens,
        positions[None, :],
        state[0],
        w_query,
        w_key,
        w_value,
        w_gate,
        w_out,
        gain_mix[None, :],
        w_ffn_gate.T,
        w_ffn_up.T,
        w_ffn_down,
        gain_out[None, :],
        jnp.asarray(inverse),
    )
    held = [pltpu.VMEM(a.shape, a.dtype) for a in arrays]
    vmem_spec = pl.BlockSpec(memory_space=pltpu.VMEM)
    any_spec = pl.BlockSpec(memory_space=pl.ANY)
    out, new_state = pl.pallas_call(
        functools.partial(step_kernel, kv_count, tp_count),
        out_shape=(
            pltpu.VMEM((rows, cols), BF16),
            pltpu.VMEM(state.shape[1:], F32),
        ),
        in_specs=[any_spec] * len(arrays),
        out_specs=(vmem_spec, vmem_spec),
        scratch_shapes=held
        + [
            pltpu.VMEM((kv_count, 4, heads, width_head), F32),
            pltpu.VMEM((kv_count, 4, heads, width_head), F32),
            pltpu.VMEM((group * heads, width_head), F32),
            pltpu.VMEM((group, rows, cols), BF16),
            pltpu.VMEM((group, rows, cols), F32),
            pltpu.VMEM((rows, width), BF16),
            pltpu.VMEM((rows, w_ffn_gate.shape[1]), BF16),
            pltpu.VMEM((group, rows, cols), BF16),
            pltpu.VMEM((group, rows, cols), BF16),
            pltpu.VMEM((group, rows, 128), F32),
            pltpu.SemaphoreType.DMA((len(arrays) + 1,)),
            pltpu.SemaphoreType.DMA((4, kv_count)),
            pltpu.SemaphoreType.DMA((4, kv_count)),
            pltpu.SemaphoreType.DMA((4, group)),
            pltpu.SemaphoreType.DMA((4, group)),
        ],
        compiler_params=pltpu.CompilerParams(
            collective_id=0, has_side_effects=True, vmem_limit_bytes=56 * 2**20
        ),
    )(*arrays)
    out, new_state = pl.pallas_call(
        store_kernel,
        out_shape=(
            jax.ShapeDtypeStruct(out.shape, out.dtype),
            jax.ShapeDtypeStruct(new_state.shape, new_state.dtype),
        ),
        in_specs=[vmem_spec, vmem_spec],
        out_specs=(any_spec, any_spec),
        scratch_shapes=[pltpu.SemaphoreType.DMA((2,))],
        compiler_params=pltpu.CompilerParams(vmem_limit_bytes=2**20),
    )(out, new_state)
    return out, new_state[None]


def fits_kernel(tokens, state, w_out, kv_count, tp_count):
    seqs, _, width_head, _ = state.shape
    return (
        seqs == 1
        and width_head == 128
        and w_out.shape[1] % 128 == 0
        and tokens.shape[0] == kv_count
        and kv_count * tp_count <= 16
    )


def rotate(vectors, positions):
    half = vectors.shape[-1] // 2
    inverse = 10000.0 ** (-jnp.arange(half, dtype=jnp.float32) / half)
    angle = positions.astype(jnp.float32)[:, None, None] * inverse[None, None, :]
    cosine = jnp.cos(angle)
    sine = jnp.sin(angle)
    first = vectors[..., :half]
    second = vectors[..., half:]
    return jnp.concatenate([first * cosine - second * sine, first * sine + second * cosine], -1)


def finish_norm(values, sums, squares, count, gain):
    mean = sums / count
    var = squares / count - mean * mean
    return (values - mean[:, None]) * lax.rsqrt(var + 1e-05)[:, None] * gain[None, :]


def on_device(
    tokens,
    positions,
    state,
    w_query,
    w_key,
    w_value,
    w_gate,
    w_out,
    gain_mix,
    w_ffn_gate,
    w_ffn_up,
    w_ffn_down,
    gain_out,
):
    if fits_kernel(tokens, state, w_out, lax.axis_size("kv"), lax.axis_size("tp")):
        return fused_step(
            tokens,
            positions,
            state,
            w_query,
            w_key,
            w_value,
            w_gate,
            w_out,
            gain_mix,
            w_ffn_gate,
            w_ffn_up,
            w_ffn_down,
            gain_out,
        )
    seqs = state.shape[0]
    heads = state.shape[1]
    width_head = state.shape[2]
    proj_cols = w_query.shape[1]
    width = w_ffn_gate.shape[0]
    cols = w_out.shape[1]
    group_rows = tokens.shape[0]
    kv_count = lax.axis_size("kv")
    tp_count = lax.axis_size("tp")
    tp_index = lax.axis_index("tp")
    col_start = (lax.axis_index("kv") * tp_count + tp_index) * cols
    projected = lax.psum_scatter(
        jnp.concatenate(
            [
                jnp.dot(tokens, w_query, preferred_element_type=jnp.float32),
                jnp.dot(tokens, w_key, preferred_element_type=jnp.float32),
                jnp.dot(tokens, w_value, preferred_element_type=jnp.float32),
                jnp.dot(tokens, w_gate, preferred_element_type=jnp.float32),
            ],
            axis=1,
        ),
        "kv",
        scatter_dimension=0,
        tiled=True,
    )
    query = projected[:, :proj_cols].reshape(seqs, heads, width_head)
    key = projected[:, proj_cols : 2 * proj_cols].reshape(seqs, heads, width_head)
    value = projected[:, 2 * proj_cols : 3 * proj_cols].reshape(seqs, heads, width_head)
    gate_pre = projected[:, 3 * proj_cols :]
    query = rotate(query, positions)
    key = rotate(key, positions) * width_head ** (-0.5)
    total_heads = heads * tp_count
    head_ids = (tp_index * heads + jnp.arange(heads, dtype=jnp.int32)).astype(jnp.float32)
    decay = 1.0 - 2.0 ** (-5.0 - 6.0 * head_ids / (total_heads - 1))
    new_state = decay[None, :, None, None] * state + key[:, :, :, None] * value[:, :, None, :]
    retained = jnp.einsum("bhd,bhdv->bhv", query, new_state, precision=lax.Precision.HIGHEST)
    mean = jnp.mean(retained, -1, keepdims=True)
    var = jnp.mean(jnp.square(retained - mean), -1, keepdims=True)
    normed = (retained - mean) * lax.rsqrt(var + 1e-05)
    attended = (normed.reshape(seqs, proj_cols) * jax.nn.silu(gate_pre)).astype(jnp.bfloat16)
    gathered = lax.all_gather(attended[None], ("kv", "tp"), axis=0, tiled=True)
    gathered = gathered.reshape(kv_count, tp_count, seqs, proj_cols)
    out_blocks = w_out.reshape(tp_count, proj_cols, cols)
    mixed = jnp.einsum(
        "itsc,tcd->isd", gathered, out_blocks, preferred_element_type=jnp.float32
    ).reshape(group_rows, cols)
    tokens_own = lax.dynamic_slice_in_dim(tokens, tp_index * cols, cols, 1)
    mixed_pre = (tokens_own.astype(jnp.float32) + mixed).astype(jnp.bfloat16)
    gain_out_own = lax.dynamic_slice_in_dim(gain_out, col_start, cols, 0)
    whole_rows = lax.all_gather(mixed_pre, ("kv", "tp"), axis=1, tiled=True).astype(jnp.float32)
    hidden = finish_norm(
        whole_rows, jnp.sum(whole_rows, 1), jnp.sum(whole_rows * whole_rows, 1), width, gain_mix
    ).astype(jnp.bfloat16)
    hidden_own = lax.dynamic_slice_in_dim(hidden, col_start, cols, 1)
    gate = jnp.dot(hidden, w_ffn_gate, preferred_element_type=jnp.float32)
    upward = jnp.dot(hidden, w_ffn_up, preferred_element_type=jnp.float32)
    inner = (jax.nn.silu(gate) * upward).astype(jnp.bfloat16)
    ffn_cols = lax.psum_scatter(
        lax.dot_general(
            w_ffn_down, inner, (((0,), (1,)), ((), ())), preferred_element_type=jnp.float32
        ),
        ("kv", "tp"),
        scatter_dimension=0,
        tiled=True,
    )
    summed = hidden_own.astype(jnp.float32) + ffn_cols.T
    out_sums, out_squares = lax.psum(
        (jnp.sum(summed, 1), jnp.sum(summed * summed, 1)), ("kv", "tp")
    )
    layer_out = finish_norm(summed, out_sums, out_squares, width, gain_out_own).astype(jnp.bfloat16)
    return (layer_out, new_state)


def solution(mesh):
    return jax.shard_map(
        on_device,
        mesh=mesh,
        in_specs=(
            P("dp", "kv"),
            P(("dp", "kv")),
            P(("dp", "kv"), "tp", None, None),
            P("kv", "tp"),
            P("kv", "tp"),
            P("kv", "tp"),
            P("kv", "tp"),
            P(None, ("kv", "tp")),
            P(),
            P(None, ("kv", "tp")),
            P(None, ("kv", "tp")),
            P(("kv", "tp"), None),
            P(),
        ),
        out_specs=(P("dp", ("kv", "tp")), P(("dp", "kv"), "tp", None, None)),
        check_vma=False,
    )
```
